256 devices in a mesh: ep: 64 (over z, y, core), tp: 4 (over x).
Axes of the slice: x: 4, y: 4, z: 8, core: 2. Of those that a mesh axis runs over, the one named last changes fastest.
Arguments:
- first_input: bfloat16 [32768, 2048], P('ep'), may hold values from -120 to 120
- first_gain: bfloat16 [2048], replicated, may hold values from 0.099609375 to 1.8984375
- pool_inward: bfloat16 [2048, 1024], P(None, 'tp'), may hold values from -0.125 to 0.125
- pool_mixing: bfloat16 [4, 256, 256], P('tp'), may hold values from -0.375 to 0.375
- pool_scale: bfloat16 [1024], P('tp'), may hold values from 0.099609375 to 1.8984375
- pool_outward: bfloat16 [1024, 2048], P('tp'), may hold values from -0.1875 to 0.1875
- second_input: bfloat16 [16384, 2048], P('ep'), may hold values from -120 to 120
- second_gain: bfloat16 [2048], replicated, may hold values from 0.099609375 to 1.8984375
- route_ids: int32 [16384, 2], P('ep'), may hold values from 0 to 31, all different within a row; in each aligned block of 256 rows (0 to 255, 256 to 511, ...) at most 18 rows name the same one
- route_logits: float32 [16384, 2], P('ep'), may hold values from -6 to 6
- expert_gate: bfloat16 [64, 2048, 2048], P('ep', None, 'tp'), may hold values from -0.125 to 0.125
- expert_up: bfloat16 [64, 2048, 2048], P('ep', None, 'tp'), may hold values from -0.125 to 0.125
- expert_down: bfloat16 [64, 2048, 2048], P('ep', 'tp'), may hold values from -0.09375 to 0.09375
Outputs:
- first_out: bfloat16 [32768, 2048], P('ep', 'tp')
- second_out: bfloat16 [16384, 2048], P('ep', 'tp')
The draws below stay inside these ranges and needn't reach their ends.
Inputs may be any that keep to these rules, and one draw needn't show every extreme that they name: `route_ids`: each row names two different experts. In each aligned block of 256 rows (the rows of one index of ep) no expert is named by more than 18 rows, and in some blocks one expert is named by exactly 18 rows.
All inputs are finite; a program needn't handle non-finite values.
Results may differ from the reference program's by a relative error of at most 0.012.
Values may be sent and summed in bfloat16 or wider, within the bound.
No kernel may reach another device: no remote copies, remote signals or barrier semaphores. Data moves between devices by JAX's collectives and lax.ppermute only.
A program may use at most 64 MiB of HBM per device.

```python
import math
import jax
import jax.numpy as jnp
import numpy as np
from jax import lax

D = 2048
POOL = 1024
FF_E = 4096
B_ROWS = 256
EXPERTS = 32
CAP = 18
TOK_A = 32768
TOK_B = 16384
N_EP = 64
N_TP = 4


def scaled_rows(key, row_count, width):
    subkeys = jax.random.split(key, 3)
    column_scale = jnp.exp(jax.random.uniform(subkeys[1], (1, width), jnp.float32, 0.0, math.log(10.0)))
    row_scale = jnp.exp(jax.random.uniform(subkeys[2], (row_count, 1), jnp.float32, 0.0, math.log(10.0)))
    values = jax.random.truncated_normal(subkeys[0], -4.0, 4.0, (row_count, width), jnp.float32)
    return (values * column_scale * row_scale * 0.25).astype(jnp.bfloat16)


def draw_first_input(key, part):
    return scaled_rows(jax.random.fold_in(key, 11), TOK_A, D)


def draw_second_input(key, part):
    return scaled_rows(jax.random.fold_in(key, 23), TOK_B, D)


def levels(own_key, extent, cuts, least, high):
    def one(position, blocks):
        steps = jax.random.uniform(jax.random.fold_in(jax.random.fold_in(own_key, 6), position), (blocks,), jnp.float32, least / len(cuts), high / len(cuts))
        return jnp.repeat(jnp.exp(steps), extent[position] // blocks).reshape((-1,) + (1,) * (len(extent) - position - 1))

    loudness = one(*cuts[0])
    for cut in cuts[1:]:
        loudness = loudness * one(*cut)
    return loudness


def assign_block(rng, own, number, rows, amount, top, reach, skew):
    order = jax.random.permutation(rng, amount)
    packed, ordinary = portions_of(amount, rows * top, reach, skew, True), portions_of(amount, rows * top, reach, skew, False)
    places = jnp.arange(amount)

    def named(tallies, turn):
        used = int((tallies > 0).sum())
        fixed = max(1, used // 4)
        shifted = fixed + (places - fixed + turn * (used - fixed)) % max(1, amount - fixed)
        return jnp.zeros((amount,), jnp.int32).at[order[jnp.where(places < fixed, places, shifted)]].set(jnp.asarray(tallies, jnp.int32))

    tallies = jnp.where(number % 4 == 0, named(packed, number // 4), named(ordinary, number - number // 4 - 1))
    mixed = jax.random.permutation(jax.random.fold_in(own, 3), amount)
    donor, sink = mixed[0:amount // 2 * 2:2], mixed[1:amount // 2 * 2:2]
    slack = jnp.minimum(tallies[donor] - 1, reach - tallies[sink]) // 2
    slack = jnp.where((donor == order[0]) | (sink == order[0]) | (tallies[sink] == 0), 0, jnp.maximum(slack, 0))
    shifted = jax.random.randint(jax.random.fold_in(own, 4), (amount // 2,), 0, 1 << 20) % (slack + 1)
    tallies = tallies.at[donor].add(-shifted).at[sink].add(shifted)
    items = jnp.searchsorted(jnp.cumsum(tallies), jnp.arange(rows * top), side="right").astype(jnp.int32)
    listing = items.reshape(top, rows).T
    listing = listing[jax.random.permutation(jax.random.fold_in(own, 1), rows)]
    turn = jax.random.randint(jax.random.fold_in(own, 2), (rows, 1), 0, top)
    return jnp.take_along_axis(listing, (jnp.arange(top)[None, :] + turn) % top, axis=1)


def portions_of(count, total, most, slope, full):
    portions = [(1 << 20) // math.isqrt(grade ** slope) + 1 for grade in range(1, count + 1)]
    largest = most if full else min(most, max(-(-total // count), total * portions[0] // sum(portions)))
    least = 1 if total - largest >= count - 1 else 0
    given, surplus = [largest] + [least] * (count - 1), total - largest - least * (count - 1)
    while surplus > 0:
        free = [i for i in range(1, count) if given[i] < largest] or [i for i in range(1, count) if given[i] < most]
        whole, left = sum([portions[i] for i in free]), surplus
        for i in free:
            extra = min(most - given[i], max(1, left * portions[i] // whole), surplus)
            given[i] = given[i] + extra
            surplus = surplus - extra
    return np.array(given)


def noise(rng, extent, scale, most, pieces=(), kind=jnp.bfloat16):
    array = scale * jax.random.normal(rng, extent, jnp.float32)
    if pieces:
        array = array * levels(rng, extent, pieces, -0.22, 0.18)
    return jnp.clip(array, -most, most).astype(kind)


def setup_inputs(seed: int = 0) -> dict:
    seeds = jax.random.split(jax.random.key(seed), 14)
    first_input = draw_first_input(jax.random.fold_in(seeds[13], 71), 0)
    first_gain = jnp.clip(1.0 + 0.18 * jax.random.normal(seeds[1], (D,), jnp.float32), 0.099609375, 1.8984375).astype(jnp.bfloat16)
    pool_inward = noise(seeds[2], (D, POOL), D ** -0.5, 0.125, ((1, 4),))
    pool_mixing = noise(seeds[3], (4, POOL // 4, POOL // 4), (POOL // 4) ** -0.5, 0.375, ((0, 4),))
    pool_scale = jnp.clip(1.0 + 0.18 * jax.random.normal(seeds[4], (POOL,), jnp.float32), 0.099609375, 1.8984375).astype(jnp.bfloat16)
    pool_outward = noise(seeds[5], (POOL, D), POOL ** -0.5, 0.1875, ((0, 4),))
    second_input = draw_second_input(jax.random.fold_in(seeds[13], 71), 0)
    second_gain = jnp.clip(1.0 + 0.18 * jax.random.normal(seeds[7], (D,), jnp.float32), 0.099609375, 1.8984375).astype(jnp.bfloat16)
    route_ids_keys = jax.random.split(jax.random.fold_in(seeds[8], 1), TOK_B // B_ROWS)
    route_ids_turns = jax.random.permutation(jax.random.fold_in(seeds[8], 3), TOK_B // B_ROWS)
    route_ids = jax.vmap(lambda own, number: assign_block(jax.random.fold_in(seeds[8], 2), own, number, B_ROWS, EXPERTS, 2, CAP, 0))(route_ids_keys, route_ids_turns).reshape((TOK_B, 2))
    route_logits = noise(seeds[9], (TOK_B, 2), 1.5, 6.0, ((0, 64),), jnp.float32)
    expert_gate = noise(seeds[10], (2 * EXPERTS, D, FF_E // 2), D ** -0.5, 0.125, ((0, 64), (2, 4)))
    expert_up = noise(seeds[11], (2 * EXPERTS, D, FF_E // 2), D ** -0.5, 0.125, ((0, 64), (2, 4)))
    expert_down = noise(seeds[12], (2 * EXPERTS, FF_E // 2, D), FF_E ** -0.5, 0.09375, ((0, 64), (1, 4)))
    return dict(first_input=first_input, first_gain=first_gain, pool_inward=pool_inward, pool_mixing=pool_mixing, pool_scale=pool_scale, pool_outward=pool_outward, second_input=second_input, second_gain=second_gain, route_ids=route_ids, route_logits=route_logits, expert_gate=expert_gate, expert_up=expert_up, expert_down=expert_down)


epsilon = 1e-06
window_lengths = (2, 4, 8, 16)

def rms_scaled(values, weights):
    widened = values.astype(jnp.float32)
    inverse = lax.rsqrt(lax.optimization_barrier(jnp.mean(widened * widened, axis=-1, keepdims=True)) + epsilon)
    return (widened * inverse * weights.astype(jnp.float32)).astype(jnp.bfloat16)

def window_means(channels, length, offset):
    row_count = channels.shape[0] - 15
    summed = jnp.zeros((row_count, channels.shape[1]), jnp.float32)
    for lookback in range(16):
        summed = summed + jnp.where(lookback < length, channels[15 - lookback:15 - lookback + row_count], 0.0)
    positions = offset + jnp.arange(row_count, dtype=jnp.int32)
    counts = jnp.minimum(positions + 1, length).astype(jnp.float32)
    return summed / counts[:, None]

def slot_positions(block_ids, expert_count, capacity):
    flattened = block_ids.reshape(-1)
    onehot = (flattened[:, None] == jnp.arange(expert_count, dtype=jnp.int32)[None, :]).astype(jnp.int32)
    running = jnp.cumsum(onehot, axis=0, dtype=jnp.int32) - 1
    slot_numbers = lax.optimization_barrier(jnp.sum(onehot * running, axis=1))
    return (flattened * capacity + slot_numbers).astype(jnp.int32)

def mixer_half(first_input, first_gain, pool_inward, pool_mixing, pool_scale, pool_outward):
    normed = rms_scaled(first_input, first_gain)
    pooled_in = jnp.dot(normed, pool_inward, preferred_element_type=jnp.float32).astype(jnp.bfloat16)
    group_width = pool_inward.shape[1] // 4
    accumulated = jnp.zeros(first_input.shape, jnp.float32)
    for group_index in range(4):
        lower = group_index * group_width
        channels = pooled_in[:, lower:lower + group_width]
        widened = jnp.pad(channels.astype(jnp.float32), ((15, 0), (0, 0)))
        means = window_means(widened, window_lengths[group_index], jnp.int32(0))
        mixed = (means - channels.astype(jnp.float32)).astype(jnp.bfloat16)
        scales = pool_scale[lower:lower + group_width].astype(jnp.float32)
        pooled = (jnp.dot(mixed, pool_mixing[group_index], preferred_element_type=jnp.float32) * scales).astype(jnp.bfloat16)
        partial_value = jnp.dot(pooled, pool_outward[lower:lower + group_width], preferred_element_type=jnp.float32).astype(jnp.bfloat16)
        accumulated = accumulated + partial_value.astype(jnp.float32)
    return accumulated.astype(jnp.bfloat16)

def block_tables(block_positions, block_shares, first_token):
    tokens = first_token + jnp.arange(2 * B_ROWS, dtype=jnp.int32) // 2
    owners = jnp.zeros((EXPERTS * CAP,), jnp.int32).at[block_positions].set(tokens)
    weights = jnp.zeros((EXPERTS * CAP,), jnp.float32).at[block_positions].set(block_shares)
    return (owners, weights)

def block_slots(block_ids):
    return slot_positions(block_ids, EXPERTS, CAP)

def expert_half(second_input, second_gain, route_ids, route_logits, expert_gate, expert_up, expert_down):
    normed = rms_scaled(second_input, second_gain)
    positions = jax.vmap(block_slots)(route_ids.reshape(N_EP, B_ROWS, 2))
    shares = jax.nn.sigmoid(route_logits - route_logits[:, ::-1])
    starts = jnp.arange(N_EP, dtype=jnp.int32) * B_ROWS
    owners, weights = jax.vmap(block_tables)(positions, shares.reshape(N_EP, 2 * B_ROWS), starts)
    owners = owners.reshape(N_EP, EXPERTS, CAP).transpose(1, 0, 2).reshape(EXPERTS, N_EP * CAP)
    weights = weights.reshape(N_EP, EXPERTS, CAP).transpose(1, 0, 2).reshape(EXPERTS, N_EP * CAP)
    half_units = expert_gate.shape[2]
    unit_group = half_units // N_TP
    gate_pairs = expert_gate.reshape(EXPERTS, 2, D, half_units)
    up_pairs = expert_up.reshape(EXPERTS, 2, D, half_units)
    down_pairs = expert_down.reshape(EXPERTS, 2, half_units, D)

    def add_expert(accumulated, inputs):
        slot_owners, slot_weights, gate_pair, up_pair, down_pair = inputs
        routed = normed[slot_owners]
        gate_full = jnp.concatenate([gate_pair[0], gate_pair[1]], axis=1)
        up_full = jnp.concatenate([up_pair[0], up_pair[1]], axis=1)
        gate_sum = jnp.dot(routed, gate_full, preferred_element_type=jnp.float32)
        up_sum = jnp.dot(routed, up_full, preferred_element_type=jnp.float32)
        hidden = (jax.nn.silu(gate_sum) * up_sum).astype(jnp.bfloat16)
        down_full = down_pair.reshape(2 * half_units, D)
        route_out = jnp.zeros((routed.shape[0], D), jnp.float32)
        for half_index in range(2):
            half_sum = jnp.zeros((routed.shape[0], D), jnp.float32)
            for quarter in range(N_TP):
                first_unit = half_index * half_units + quarter * unit_group
                product = jnp.dot(hidden[:, first_unit:first_unit + unit_group], down_full[first_unit:first_unit + unit_group], preferred_element_type=jnp.float32).astype(jnp.bfloat16)
                half_sum = half_sum + product.astype(jnp.float32)
            route_out = route_out + half_sum.astype(jnp.bfloat16).astype(jnp.float32)
        return (accumulated.at[slot_owners].add(slot_weights[:, None] * route_out), None)
    accumulated, unused = lax.scan(add_expert, jnp.zeros((second_input.shape[0], D), jnp.float32), (owners, weights, gate_pairs, up_pairs, down_pairs))
    return accumulated.astype(jnp.bfloat16)

def reference(first_input, first_gain, pool_inward, pool_mixing, pool_scale, pool_outward, second_input, second_gain, route_ids, route_logits, expert_gate, expert_up, expert_down):
    first_out = mixer_half(first_input, first_gain, pool_inward, pool_mixing, pool_scale, pool_outward)
    second_out = expert_half(second_input, second_gain, route_ids, route_logits, expert_gate, expert_up, expert_down)
    return (first_out, second_out)
```

```python
import jax
import jax.numpy as jnp
from jax import lax
from jax.sharding import Mesh, PartitionSpec as P

epsilon = 1e-06


def from_behind(value, axis, steps):
    count = lax.axis_size(axis)
    leading, last = (max(0, -steps), min(count, count - steps))
    return lax.ppermute(value, axis, [(source, source + steps) for source in range(leading, last)])


def rms_scaled(values, weights):
    widened = values.astype(jnp.float32)
    inverse = lax.rsqrt(jnp.mean(widened * widened, axis=-1, keepdims=True) + epsilon)
    return (widened * inverse * weights.astype(jnp.float32)).astype(jnp.bfloat16)


def window_means(channels, length, offset):
    row_count = channels.shape[0] - 15
    summed = jnp.zeros((row_count, channels.shape[1]), jnp.float32)
    for lookback in range(16):
        summed = summed + jnp.where(
            lookback < length, channels[15 - lookback : 15 - lookback + row_count], 0.0
        )
    positions = offset + jnp.arange(row_count, dtype=jnp.int32)
    counts = jnp.minimum(positions + 1, length).astype(jnp.float32)
    return summed / counts[:, None]


def slot_positions(block_ids, expert_count, capacity):
    flattened = block_ids.reshape(-1)
    onehot = (flattened[:, None] == jnp.arange(expert_count, dtype=jnp.int32)[None, :]).astype(
        jnp.int32
    )
    running = jnp.cumsum(onehot, axis=0, dtype=jnp.int32) - 1
    slot_numbers = jnp.sum(onehot * running, axis=1)
    return flattened * capacity + slot_numbers


def expert_output(gate_sum, up_sum, down_rows):
    hidden = (jax.nn.silu(gate_sum) * up_sum).astype(jnp.bfloat16)
    return jnp.dot(hidden, down_rows, preferred_element_type=jnp.float32)


def local(
    first_input,
    first_gain,
    pool_inward,
    pool_mixing,
    pool_scale,
    pool_outward,
    second_input,
    second_gain,
    route_ids,
    route_logits,
    expert_gate,
    expert_up,
    expert_down,
):
    tensor_parts = lax.axis_size("tp")
    expert_count = lax.axis_size("z") * lax.axis_size("y")
    model_width = first_input.shape[1]
    quarter_width = model_width // tensor_parts
    swap = [(0, 1), (1, 0)]
    gate_other = lax.ppermute(expert_gate[0], "core", swap)
    up_other = lax.ppermute(expert_up[0], "core", swap)
    down_other = lax.ppermute(expert_down[0], "core", swap)
    normed_first = rms_scaled(first_input, first_gain)
    pooled_in = jnp.dot(normed_first, pool_inward, preferred_element_type=jnp.float32).astype(
        jnp.bfloat16
    )
    halo_rows = from_behind(pooled_in[-15:], ("z", "y", "core"), 1)
    extended = jnp.concatenate([halo_rows, pooled_in], axis=0).astype(jnp.float32)
    window = jnp.left_shift(jnp.int32(2), lax.axis_index("tp"))
    sequence_start = lax.axis_index(("z", "y", "core")) * first_input.shape[0]
    means = window_means(extended, window, sequence_start)
    mixed = (means - pooled_in.astype(jnp.float32)).astype(jnp.bfloat16)
    pooled = (
        jnp.dot(mixed, pool_mixing[0], preferred_element_type=jnp.float32)
        * pool_scale.astype(jnp.float32)
    ).astype(jnp.bfloat16)
    mixer_term = jnp.dot(pooled, pool_outward, preferred_element_type=jnp.float32)
    normed_second = rms_scaled(second_input, second_gain)
    row_count = second_input.shape[0]
    capacity = 2 * row_count * 9 // (8 * expert_count)
    positions = slot_positions(route_ids, expert_count, capacity)
    quarter = lax.dynamic_slice_in_dim(
        normed_second, lax.axis_index("tp") * quarter_width, quarter_width, 1
    )
    repeated = jnp.repeat(quarter, 2, axis=0)
    buffer = (
        jnp.zeros((expert_count * capacity, quarter_width), jnp.bfloat16)
        .at[positions]
        .set(repeated)
    ).reshape(expert_count, capacity, quarter_width)
    arrived = lax.all_to_all(buffer, ("z", "y"), split_axis=0, concat_axis=0, tiled=True)
    flattened = arrived.reshape(-1, quarter_width)
    portion = lax.all_gather(flattened, "tp", axis=1, tiled=True)
    flat_term = expert_output(
        jnp.dot(portion, expert_gate[0], preferred_element_type=jnp.float32),
        jnp.dot(portion, expert_up[0], preferred_element_type=jnp.float32),
        expert_down[0],
    ) + expert_output(
        jnp.dot(portion, gate_other, preferred_element_type=jnp.float32),
        jnp.dot(portion, up_other, preferred_element_type=jnp.float32),
        down_other,
    )
    first_out = lax.psum_scatter(
        mixer_term.astype(jnp.bfloat16), "tp", scatter_dimension=1, tiled=True
    )
    expert_summed = lax.psum_scatter(
        flat_term.astype(jnp.bfloat16), "tp", scatter_dimension=1, tiled=True
    )
    half_out = expert_summed.reshape(expert_count, capacity, quarter_width)
    returned = lax.all_to_all(half_out, ("z", "y"), split_axis=0, concat_axis=0, tiled=True)
    route_out = returned.reshape(-1, quarter_width).astype(jnp.float32)
    picked = route_out[positions].reshape(row_count, 2, quarter_width)
    shares = jax.nn.sigmoid(route_logits - route_logits[:, ::-1])
    second_out = jnp.sum(picked * shares[:, :, None], axis=1).astype(jnp.bfloat16)
    return (first_out, second_out)


def solution(mesh):
    split_mesh = Mesh(mesh.devices.reshape(8, 4, 2, 4), ("z", "y", "core", "tp"))
    ep = ("z", "y", "core")
    placed = (
        P(ep, None),
        P(),
        P(None, "tp"),
        P("tp", None, None),
        P("tp"),
        P("tp", None),
        P(ep, None),
        P(),
        P(ep, None),
        P(ep, None),
        P(ep, None, "tp"),
        P(ep, None, "tp"),
        P(ep, "tp", None),
    )
    return jax.shard_map(
        local,
        mesh=split_mesh,
        in_specs=placed,
        out_specs=(P(ep, "tp"), P(ep, "tp")),
        check_vma=False,
    )
```

```python
import jax
import jax.numpy as jnp
from jax import lax
from jax.experimental import pallas as pl
from jax.experimental.pallas import tpu as pltpu
from jax.sharding import Mesh, PartitionSpec as P

epsilon = 1e-06
EP = ("z", "y", "core")
ZY = ("z", "y")
LANES = 128
MAIN = 16
f32 = jnp.float32
bf16 = jnp.bfloat16


def shifted(value, axis, steps):
    count = lax.axis_size(axis)
    return lax.ppermute(value, axis, [(i, (i + steps) % count) for i in range(count)])


def from_behind(value, axis, steps):
    count = lax.axis_size(axis)
    leading, last = (max(0, -steps), min(count, count - steps))
    return lax.ppermute(value, axis, [(source, source + steps) for source in range(leading, last)])


def rms_scaled(values, weights):
    widened = values.astype(f32)
    inverse = lax.rsqrt(jnp.mean(widened * widened, axis=-1, keepdims=True) + epsilon)
    return (widened * inverse * weights.astype(f32)).astype(bf16)


def window_means(channels, length, offset):
    row_count = channels.shape[0] - 15
    summed = jnp.zeros((row_count, channels.shape[1]), f32)
    for lookback in range(16):
        summed = summed + jnp.where(
            lookback < length, channels[15 - lookback : 15 - lookback + row_count], 0.0
        )
    positions = offset + jnp.arange(row_count, dtype=jnp.int32)
    counts = jnp.minimum(positions + 1, length).astype(f32)
    return summed / counts[:, None]


def iota(shape, dim):
    return lax.broadcasted_iota(jnp.int32, shape, dim)


def dot(a, b):
    return jnp.dot(a, b, preferred_element_type=f32)


def head_kernel(part_ref, x_ref, gain_ref, ids_ref, out_ref):
    tokens, width = x_ref.shape
    experts = out_ref.shape[0]
    quarter = width // 4
    total = jnp.zeros((tokens, 1), f32)
    for lower in range(0, width, quarter):
        piece = x_ref[:, lower : lower + quarter].astype(f32)
        total = total + jnp.sum(piece * piece, axis=1, keepdims=True)
    inverse = lax.rsqrt(total / width + epsilon)
    start = pl.multiple_of(part_ref[0] * quarter, quarter)
    mine = x_ref[:, pl.ds(start, quarter)].astype(f32)
    normed = (mine * inverse * gain_ref[:, pl.ds(start, quarter)].astype(f32)).astype(bf16)
    named = iota((experts, tokens), 0)
    member = (ids_ref[0:1, :] == named) | (ids_ref[1:2, :] == named)
    earlier = (iota((tokens, tokens), 0) < iota((tokens, tokens), 1)).astype(f32).astype(bf16)
    rank = dot(member.astype(f32).astype(bf16), earlier)
    code = jnp.where(member, rank, -1.0).astype(bf16)
    rows = experts * MAIN
    spread = (iota((rows, experts), 0) // MAIN == iota((rows, experts), 1)).astype(f32).astype(bf16)
    slot = (iota((rows, tokens), 0) % MAIN).astype(f32)
    chosen = (dot(spread, code) == slot).astype(f32).astype(bf16)
    main = dot(chosen, normed).astype(bf16)
    tiles = quarter // LANES
    for tile in range(tiles):
        out_ref[:, tile * MAIN : (tile + 1) * MAIN, :] = main[
            :, tile * LANES : (tile + 1) * LANES
        ].reshape(experts, MAIN, LANES)
    rest = 2 * tiles
    rows = experts * rest
    spread = (iota((rows, experts), 0) // rest == iota((rows, experts), 1)).astype(f32).astype(bf16)
    expanded = dot(spread, code)
    place = iota((rows, tokens), 0)
    hit = expanded == (MAIN + place % 2).astype(f32)
    summed = jnp.zeros((rows, LANES), f32)
    for tile in range(tiles):
        chosen = (hit & ((place % rest) // 2 == tile)).astype(f32).astype(bf16)
        summed = summed + dot(chosen, normed[:, tile * LANES : (tile + 1) * LANES])
    out_ref[:, tiles * MAIN :, :] = summed.reshape(experts, rest, LANES).astype(bf16)


def rest_order(sources, tiles, flip):
    size = sources * tiles * 2
    outer, inner = iota((size, size), 0), iota((size, size), 1)
    if flip:
        outer, inner = inner, outer
    tile, source, slot = outer // (2 * sources), (outer % (2 * sources)) // 2, outer % 2
    return (inner == source * 2 * tiles + tile * 2 + slot).astype(f32).astype(bf16)


def expert_kernel(
    part_ref, own_ref, la_ref, lb_ref, ra_ref, rb_ref, oa_ref, ob_ref,
    g0_hbm, u0_hbm, d0_hbm, g1_hbm, u1_hbm, d1_hbm,
    own_out, ra_out, rb_out, la_out, lb_out, oa_out, ob_out,
    x_ref, g_ref, u_ref, d_ref, sems,
):
    sources = own_ref.shape[0]
    half = sources // 2
    units = g_ref.shape[2]
    quarter = 4 * LANES
    tiles = 4
    copies = []
    for index, (source, target) in enumerate(
        (
            (g0_hbm, g_ref.at[0]),
            (u0_hbm, u_ref.at[0]),
            (g1_hbm, g_ref.at[1]),
            (u1_hbm, u_ref.at[1]),
            (d0_hbm, d_ref.at[pl.ds(0, units)]),
            (d1_hbm, d_ref.at[pl.ds(units, units)]),
        )
    ):
        copy = pltpu.make_async_copy(source, target, sems.at[index])
        copy.start()
        copies.append(copy)
    part = part_ref[0]
    starts = [
        pl.multiple_of(((part + shift) % 4) * quarter, quarter) for shift in (0, 3, 1, 2)
    ]
    groups = (
        ((own_ref, 0, half), (own_ref, half, half)),
        ((la_ref, 0, half), (lb_ref, 0, half)),
        ((ra_ref, 0, half), (rb_ref, 0, half)),
        ((oa_ref, 0, half), (ob_ref, 0, half)),
    )
    main_rows = sources * MAIN
    rests = []
    for start, pair in zip(starts, groups):
        rest = []
        for side, (ref, first, count) in enumerate(pair):
            rows = count * MAIN
            for tile in range(tiles):
                block = ref[first : first + count, tile * MAIN : (tile + 1) * MAIN, :]
                x_ref[side * rows : (side + 1) * rows, pl.ds(start + tile * LANES, LANES)] = (
                    block.reshape(rows, LANES)
                )
            rest.append(ref[first : first + count, tiles * MAIN :, :].astype(f32))
        rests.append(
            jnp.concatenate(rest, axis=0).reshape(sources * 2 * tiles, LANES).astype(bf16)
        )
    moved = dot(rest_order(sources, tiles, False), jnp.concatenate(rests, axis=1)).astype(bf16)
    for index, start in enumerate(starts):
        for tile in range(tiles):
            x_ref[main_rows:, pl.ds(start + tile * LANES, LANES)] = moved[
                tile * 2 * sources : (tile + 1) * 2 * sources,
                index * LANES : (index + 1) * LANES,
            ]
    x = x_ref[...]
    hidden = []
    for side in range(2):
        copies[2 * side].wait()
        gate = dot(x, g_ref[side])
        copies[2 * side + 1].wait()
        up = dot(x, u_ref[side])
        hidden.append((gate / (1.0 + jnp.exp(-gate)) * up).astype(bf16))
    hidden = jnp.concatenate(hidden, axis=1)
    copies[4].wait()
    copies[5].wait()
    targets = (
        ((own_out, 0), (own_out, half)),
        ((la_out, 0), (lb_out, 0)),
        ((ra_out, 0), (rb_out, 0)),
        ((oa_out, 0), (ob_out, 0)),
    )
    rests = []
    for start, pair in zip(starts, targets):
        result = dot(hidden, d_ref[:, pl.ds(start, quarter)]).astype(bf16)
        rows = half * MAIN
        for side, (ref, first) in enumerate(pair):
            for tile in range(tiles):
                ref[first : first + half, tile * MAIN : (tile + 1) * MAIN, :] = result[
                    side * rows : (side + 1) * rows, tile * LANES : (tile + 1) * LANES
                ].reshape(half, MAIN, LANES)
        rests.append(
            jnp.concatenate(
                [result[main_rows:, tile * LANES : (tile + 1) * LANES] for tile in range(tiles)],
                axis=0,
            )
        )
    moved = dot(rest_order(sources, tiles, True), jnp.concatenate(rests, axis=1))
    for index, pair in enumerate(targets):
        block = moved[:, index * LANES : (index + 1) * LANES].reshape(sources, 2 * tiles, LANES)
        for side, (ref, first) in enumerate(pair):
            ref[first : first + half, tiles * MAIN :, :] = block[
                side * half : (side + 1) * half
            ].astype(bf16)


def tail_kernel(back_ref, ids_ref, shares_ref, out_ref):
    tokens, quarter = out_ref.shape
    experts = back_ref.shape[0]
    tiles = quarter // LANES
    rest = 2 * tiles
    named = iota((tokens, experts), 1)
    members = [ids_ref[:, k : k + 1] == named for k in range(2)]
    earlier = (iota((tokens, tokens), 1) < iota((tokens, tokens), 0)).astype(f32).astype(bf16)
    rank = dot(earlier, (members[0] | members[1]).astype(f32).astype(bf16))
    rows = experts * MAIN
    spread_main = (
        (iota((experts, rows), 1) // MAIN == iota((experts, rows), 0)).astype(f32).astype(bf16)
    )
    slot_main = (iota((tokens, rows), 1) % MAIN).astype(f32)
    rest_rows = experts * rest
    spread_rest = (
        (iota((experts, rest_rows), 1) // rest == iota((experts, rest_rows), 0))
        .astype(f32)
        .astype(bf16)
    )
    place = iota((tokens, rest_rows), 1)
    slot_rest = (MAIN + place % 2).astype(f32)
    main = jnp.concatenate(
        [
            back_ref[:, tile * MAIN : (tile + 1) * MAIN, :].reshape(rows, LANES)
            for tile in range(tiles)
        ],
        axis=1,
    )
    last = back_ref[:, tiles * MAIN :, :].astype(f32).reshape(rest_rows, LANES).astype(bf16)
    total = jnp.zeros((tokens, quarter), f32)
    for k in range(2):
        code = jnp.where(members[k], rank, -1.0).astype(bf16)
        chosen = (dot(code, spread_main) == slot_main).astype(f32).astype(bf16)
        picked = dot(chosen, main)
        hit = dot(code, spread_rest) == slot_rest
        extra = jnp.concatenate(
            [
                dot((hit & ((place % rest) // 2 == tile)).astype(f32).astype(bf16), last)
                for tile in range(tiles)
            ],
            axis=1,
        )
        total = total + shares_ref[:, k : k + 1] * (picked + extra)
    out_ref[...] = total.astype(bf16)


VMEM = pl.BlockSpec(memory_space=pltpu.VMEM)
SMEM = pl.BlockSpec(memory_space=pltpu.SMEM)
ANY = pl.BlockSpec(memory_space=pl.ANY)
LARGE = pltpu.CompilerParams(vmem_limit_bytes=52 * 1024 * 1024)
SMALL = pltpu.CompilerParams(vmem_limit_bytes=24 * 1024 * 1024)


def local(
    first_input,
    first_gain,
    pool_inward,
    pool_mixing,
    pool_scale,
    pool_outward,
    second_input,
    second_gain,
    route_ids,
    route_logits,
    expert_gate,
    expert_up,
    expert_down,
):
    experts = lax.axis_size("z") * lax.axis_size("y")
    width = first_input.shape[1]
    quarter = width // 4
    units = expert_gate.shape[2]
    tokens = second_input.shape[0]
    part = lax.axis_index("tp")
    part_array = part.reshape(1)
    message = jax.ShapeDtypeStruct((experts, 72, LANES), bf16)
    half_message = jax.ShapeDtypeStruct((experts // 2, 72, LANES), bf16)
    half = experts // 2

    swap = [(0, 1), (1, 0)]
    sent = pl.pallas_call(
        head_kernel,
        out_shape=message,
        in_specs=[SMEM, VMEM, VMEM, VMEM],
        out_specs=VMEM,
        compiler_params=SMALL,
        name="dispatch_rows",
    )(part_array, second_input, second_gain.reshape(1, width), route_ids.T)
    arrived = lax.all_to_all(sent, ZY, split_axis=0, concat_axis=0, tiled=True)
    gate_other = lax.ppermute(expert_gate[0], "core", swap)
    up_other = lax.ppermute(expert_up[0], "core", swap)
    down_other = lax.ppermute(expert_down[0], "core", swap)

    normed_first = rms_scaled(first_input, first_gain)
    pooled_in = dot(normed_first, pool_inward).astype(bf16)
    halo_rows = from_behind(pooled_in[-15:], EP, 1)
    extended = jnp.concatenate([halo_rows, pooled_in], axis=0).astype(f32)
    window = jnp.left_shift(jnp.int32(2), part)
    sequence_start = lax.axis_index(EP) * first_input.shape[0]
    means = window_means(extended, window, sequence_start)
    mixed = (means - pooled_in.astype(f32)).astype(bf16)
    pooled = (dot(mixed, pool_mixing[0]) * pool_scale.astype(f32)).astype(bf16)
    outward = [
        lax.dynamic_slice_in_dim(pool_outward, ((part + shift) % 4) * quarter, quarter, 1)
        for shift in range(4)
    ]
    outward = [outward[0]] + [shifted(outward[shift], "tp", shift) for shift in (1, 2, 3)]

    first, second = arrived[:half], arrived[half:]
    left_a = shifted(first, "tp", 1)
    right_b = shifted(second, "tp", -1)
    left_b = shifted(second, "tp", 1)
    right_a = shifted(first, "tp", -1)
    over_a = shifted(left_a, "tp", 1)
    over_b = shifted(right_b, "tp", -1)

    outs = pl.pallas_call(
        expert_kernel,
        out_shape=(message,) + (half_message,) * 6,
        in_specs=[SMEM] + [VMEM] * 7 + [ANY] * 6,
        out_specs=(VMEM,) * 7,
        scratch_shapes=[
            pltpu.VMEM((experts * 18, width), bf16),
            pltpu.VMEM((2, width, units), bf16),
            pltpu.VMEM((2, width, units), bf16),
            pltpu.VMEM((2 * units, width), bf16),
            pltpu.SemaphoreType.DMA((6,)),
        ],
        compiler_params=LARGE,
        cost_estimate=pl.CostEstimate(
            flops=12 * experts * 18 * width * units, bytes_accessed=18 << 20, transcendentals=0
        ),
        name="expert_units",
    )(
        part_array, arrived, left_a, left_b, right_a, right_b, over_a, over_b,
        expert_gate[0], expert_up[0], expert_down[0], gate_other, up_other, down_other,
    )
    own, to_right_a, to_right_b, to_left_a, to_left_b, to_over_a, to_over_b = outs

    passing_a = shifted(to_over_a, "tp", 1)
    passing_b = shifted(to_over_b, "tp", -1)
    from_left_b = shifted(to_right_b, "tp", 1)
    from_right_a = shifted(to_left_a, "tp", -1)
    from_left_a = shifted((to_right_a.astype(f32) + passing_a.astype(f32)).astype(bf16), "tp", 1)
    from_right_b = shifted((to_left_b.astype(f32) + passing_b.astype(f32)).astype(bf16), "tp", -1)
    summed = jnp.concatenate(
        [
            own[:half].astype(f32) + from_left_a.astype(f32) + from_right_a.astype(f32),
            own[half:].astype(f32) + from_left_b.astype(f32) + from_right_b.astype(f32),
        ],
        axis=0,
    ).astype(bf16)
    back = lax.all_to_all(summed, ZY, split_axis=0, concat_axis=0, tiled=True)

    pooled, summed_tie = lax.optimization_barrier((pooled, summed[0, 0, 0]))
    terms = [dot(pooled, outward[0])] + [
        dot(shifted(pooled, "tp", shift), outward[shift]) for shift in (1, 2, 3)
    ]
    first_out = ((terms[0] + terms[1]) + (terms[2] + terms[3])).astype(bf16)

    shares = jax.nn.sigmoid(route_logits - route_logits[:, ::-1])
    second_out = pl.pallas_call(
        tail_kernel,
        out_shape=jax.ShapeDtypeStruct((tokens, quarter), bf16),
        in_specs=[VMEM] * 3,
        out_specs=VMEM,
        compiler_params=SMALL,
        name="combine_rows",
    )(back, route_ids, shares)
    return (first_out, second_out)


def solution(mesh):
    split_mesh = Mesh(mesh.devices.reshape(8, 4, 2, 4), ("z", "y", "core", "tp"))
    placed = (
        P(EP, None),
        P(),
        P(None, "tp"),
        P("tp", None, None),
        P("tp"),
        P("tp", None),
        P(EP, None),
        P(),
        P(EP, None),
        P(EP, None),
        P(EP, None, "tp"),
        P(EP, None, "tp"),
        P(EP, "tp", None),
    )
    return jax.shard_map(
        local,
        mesh=split_mesh,
        in_specs=placed,
        out_specs=(P(EP, "tp"), P(EP, "tp")),
        check_vma=False,
    )
```

```python
import functools

import jax
import jax.numpy as jnp
from jax import lax
from jax.experimental import pallas as pl
from jax.experimental.pallas import tpu as pltpu
from jax.sharding import Mesh, PartitionSpec as P

epsilon = 1e-06
EP = ("z", "y", "core")
ZY = ("z", "y")
LANES = 128
MAIN = 16
HALO = 16
f32 = jnp.float32
bf16 = jnp.bfloat16


def shifted(value, axis, steps):
    count = lax.axis_size(axis)
    return lax.ppermute(value, axis, [(i, (i + steps) % count) for i in range(count)])


def from_behind(value, axis, steps):
    count = lax.axis_size(axis)
    leading, last = (max(0, -steps), min(count, count - steps))
    return lax.ppermute(value, axis, [(source, source + steps) for source in range(leading, last)])


def iota(shape, dim):
    return lax.broadcasted_iota(jnp.int32, shape, dim)


def dot(a, b):
    return jnp.dot(a, b, preferred_element_type=f32)


def head_kernel(part_ref, x_ref, gain_ref, ids_ref, out_ref):
    tokens, width = x_ref.shape
    experts = out_ref.shape[0]
    quarter = width // 4
    total = jnp.zeros((tokens, 1), f32)
    for lower in range(0, width, quarter):
        piece = x_ref[:, lower : lower + quarter].astype(f32)
        total = total + jnp.sum(piece * piece, axis=1, keepdims=True)
    inverse = lax.rsqrt(total / width + epsilon)
    start = pl.multiple_of(part_ref[0] * quarter, quarter)
    mine = x_ref[:, pl.ds(start, quarter)].astype(f32)
    normed = (mine * inverse * gain_ref[:, pl.ds(start, quarter)].astype(f32)).astype(bf16)
    named = iota((experts, tokens), 0)
    member = (ids_ref[0:1, :] == named) | (ids_ref[1:2, :] == named)
    earlier = (iota((tokens, tokens), 0) < iota((tokens, tokens), 1)).astype(f32).astype(bf16)
    rank = dot(member.astype(f32).astype(bf16), earlier)
    code = jnp.where(member, rank, -1.0).astype(bf16)
    rows = experts * MAIN
    spread = (iota((rows, experts), 0) // MAIN == iota((rows, experts), 1)).astype(f32).astype(bf16)
    slot = (iota((rows, tokens), 0) % MAIN).astype(f32)
    chosen = (dot(spread, code) == slot).astype(f32).astype(bf16)
    main = dot(chosen, normed).astype(bf16)
    tiles = quarter // LANES
    for tile in range(tiles):
        out_ref[:, tile * MAIN : (tile + 1) * MAIN, :] = main[
            :, tile * LANES : (tile + 1) * LANES
        ].reshape(experts, MAIN, LANES)
    rest = 2 * tiles
    rows = experts * rest
    spread = (iota((rows, experts), 0) // rest == iota((rows, experts), 1)).astype(f32).astype(bf16)
    expanded = dot(spread, code)
    place = iota((rows, tokens), 0)
    hit = expanded == (MAIN + place % 2).astype(f32)
    summed = jnp.zeros((rows, LANES), f32)
    for tile in range(tiles):
        chosen = (hit & ((place % rest) // 2 == tile)).astype(f32).astype(bf16)
        summed = summed + dot(chosen, normed[:, tile * LANES : (tile + 1) * LANES])
    out_ref[:, tiles * MAIN :, :] = summed.reshape(experts, rest, LANES).astype(bf16)


def rest_order(sources, tiles, flip):
    size = sources * tiles * 2
    outer, inner = iota((size, size), 0), iota((size, size), 1)
    if flip:
        outer, inner = inner, outer
    tile, source, slot = outer // (2 * sources), (outer % (2 * sources)) // 2, outer % 2
    return (inner == source * 2 * tiles + tile * 2 + slot).astype(f32).astype(bf16)


def gathered_rows(x_ref, groups, sources):
    tiles = 4
    quarter = tiles * LANES
    half = sources // 2
    main_rows = sources * MAIN
    rests = []
    for index, pair in enumerate(groups):
        rest = []
        for side, (ref, first) in enumerate(pair):
            rows = half * MAIN
            for tile in range(tiles):
                block = ref[first : first + half, tile * MAIN : (tile + 1) * MAIN, :]
                lower = index * quarter + tile * LANES
                x_ref[side * rows : (side + 1) * rows, lower : lower + LANES] = block.reshape(
                    rows, LANES
                )
            rest.append(ref[first : first + half, tiles * MAIN :, :].astype(f32))
        rests.append(
            jnp.concatenate(rest, axis=0).reshape(sources * 2 * tiles, LANES).astype(bf16)
        )
    moved = dot(rest_order(sources, tiles, False), jnp.concatenate(rests, axis=1)).astype(bf16)
    for index in range(len(groups)):
        for tile in range(tiles):
            lower = index * quarter + tile * LANES
            x_ref[main_rows:, lower : lower + LANES] = moved[
                tile * 2 * sources : (tile + 1) * 2 * sources,
                index * LANES : (index + 1) * LANES,
            ]


def near_kernel(shifts, *refs):
    count = len(shifts)
    part_ref = refs[0]
    groups, place = [], 1
    for shift in shifts:
        if shift == 0:
            groups.append(((refs[place], 0), (refs[place], refs[place].shape[0] // 2)))
            place += 1
        else:
            groups.append(((refs[place], 0), (refs[place + 1], 0)))
            place += 2
    earlier_ref = None
    if shifts[0] != 0:
        earlier_ref = refs[place]
        place += 1
    g0_ref, u0_ref, g1_hbm, u1_hbm, sum_ref, x_ref, g1_ref, u1_ref, sems = refs[place:]
    quarter = 4 * LANES
    part = part_ref[0]
    starts = [pl.multiple_of(((part + shift) % 4) * quarter, quarter) for shift in shifts]
    copies = []
    for side, (source, target) in enumerate(((g1_hbm, g1_ref), (u1_hbm, u1_ref))):
        for index, start in enumerate(starts):
            copies.append(
                pltpu.make_async_copy(
                    source.at[pl.ds(start, quarter)],
                    target.at[pl.ds(index * quarter, quarter)],
                    sems.at[side * count + index],
                )
            )
    for copy in copies:
        copy.start()
    gathered_rows(x_ref, groups, x_ref.shape[0] // 18)
    for index in range(4):
        if index >= 2:
            for copy in copies[(index - 2) * count : (index - 1) * count]:
                copy.wait()
        total = None if earlier_ref is None else earlier_ref[index]
        for at, start in enumerate(starts):
            if index < 2:
                rows = (g0_ref, u0_ref)[index][pl.ds(start, quarter), :]
            else:
                rows = (g1_ref, u1_ref)[index - 2][at * quarter : (at + 1) * quarter, :]
            term = dot(x_ref[:, at * quarter : (at + 1) * quarter], rows)
            total = term if total is None else total + term
        sum_ref[index] = total


def far_kernel(
    part_ref, oa_ref, ob_ref, sum_ref, g0_ref, u0_ref, g1_hbm, u1_hbm, d0_ref, d1_hbm,
    own_out, ra_out, rb_out, la_out, lb_out, oa_out, ob_out,
    x_ref, hidden_ref, g1_ref, u1_ref, d1_ref, sems,
):
    half = oa_ref.shape[0]
    sources = 2 * half
    tiles = 4
    quarter = tiles * LANES
    units = g0_ref.shape[1]
    main_rows = sources * MAIN
    part = part_ref[0]
    starts = [pl.multiple_of(((part + shift) % 4) * quarter, quarter) for shift in (2, 3, 1, 0)]
    far = pl.ds(starts[0], quarter)
    copies = [
        pltpu.make_async_copy(g1_hbm.at[far], g1_ref, sems.at[0]),
        pltpu.make_async_copy(u1_hbm.at[far], u1_ref, sems.at[1]),
        pltpu.make_async_copy(d1_hbm, d1_ref, sems.at[2]),
    ]
    for copy in copies:
        copy.start()
    gathered_rows(x_ref, (((oa_ref, 0), (ob_ref, 0)),), sources)
    x = x_ref[...]
    for side in range(2):
        if side == 0:
            gate_rows, up_rows = g0_ref[far, :], u0_ref[far, :]
        else:
            copies[0].wait()
            copies[1].wait()
            gate_rows, up_rows = g1_ref[...], u1_ref[...]
        gate = sum_ref[2 * side] + dot(x, gate_rows)
        up = sum_ref[2 * side + 1] + dot(x, up_rows)
        hidden_ref[:, side * units : (side + 1) * units] = (
            gate / (1.0 + jnp.exp(-gate)) * up
        ).astype(bf16)
    copies[2].wait()
    targets = (
        ((oa_out, 0), (ob_out, 0)),
        ((la_out, 0), (lb_out, 0)),
        ((ra_out, 0), (rb_out, 0)),
        ((own_out, 0), (own_out, half)),
    )
    rests = []
    for start, pair in zip(starts, targets):
        result = (
            dot(hidden_ref[:, :units], d0_ref[:, pl.ds(start, quarter)])
            + dot(hidden_ref[:, units:], d1_ref[:, pl.ds(start, quarter)])
        ).astype(bf16)
        rows = half * MAIN
        for side, (ref, first) in enumerate(pair):
            for tile in range(tiles):
                ref[first : first + half, tile * MAIN : (tile + 1) * MAIN, :] = result[
                    side * rows : (side + 1) * rows, tile * LANES : (tile + 1) * LANES
                ].reshape(half, MAIN, LANES)
        rests.append(
            jnp.concatenate(
                [result[main_rows:, tile * LANES : (tile + 1) * LANES] for tile in range(tiles)],
                axis=0,
            )
        )
    moved = dot(rest_order(sources, tiles, True), jnp.concatenate(rests, axis=1))
    for index, pair in enumerate(targets):
        block = moved[:, index * LANES : (index + 1) * LANES].reshape(sources, 2 * tiles, LANES)
        for side, (ref, first) in enumerate(pair):
            ref[first : first + half, tiles * MAIN :, :] = block[
                side * half : (side + 1) * half
            ].astype(bf16)


def tail_kernel(
    back_ref, ids_ref, logits_ref, t0_ref, t1_ref, t2_ref, t3_ref, first_ref, out_ref
):
    first_ref[...] = (
        (t0_ref[...].astype(f32) + t1_ref[...].astype(f32))
        + (t2_ref[...].astype(f32) + t3_ref[...].astype(f32))
    ).astype(bf16)
    logits = logits_ref[...]
    shares = jax.nn.sigmoid(logits - jnp.concatenate([logits[1:2], logits[0:1]], axis=0))
    rows = jnp.concatenate(
        [ids_ref[...].astype(f32), shares, jnp.zeros((4, logits.shape[1]), f32)], axis=0
    )
    columns = jnp.transpose(rows)
    tokens, quarter = out_ref.shape
    experts = back_ref.shape[0]
    tiles = quarter // LANES
    rest = 2 * tiles
    named = iota((tokens, experts), 1)
    members = [columns[:, k : k + 1] == named.astype(f32) for k in range(2)]
    earlier = (iota((tokens, tokens), 1) < iota((tokens, tokens), 0)).astype(f32).astype(bf16)
    rank = dot(earlier, (members[0] | members[1]).astype(f32).astype(bf16))
    rows = experts * MAIN
    spread_main = (
        (iota((experts, rows), 1) // MAIN == iota((experts, rows), 0)).astype(f32).astype(bf16)
    )
    slot_main = (iota((tokens, rows), 1) % MAIN).astype(f32)
    rest_rows = experts * rest
    spread_rest = (
        (iota((experts, rest_rows), 1) // rest == iota((experts, rest_rows), 0))
        .astype(f32)
        .astype(bf16)
    )
    place = iota((tokens, rest_rows), 1)
    slot_rest = (MAIN + place % 2).astype(f32)
    main = jnp.concatenate(
        [
            back_ref[:, tile * MAIN : (tile + 1) * MAIN, :].reshape(rows, LANES)
            for tile in range(tiles)
        ],
        axis=1,
    )
    last = back_ref[:, tiles * MAIN :, :].astype(f32).reshape(rest_rows, LANES).astype(bf16)
    total = jnp.zeros((tokens, quarter), f32)
    for k in range(2):
        code = jnp.where(members[k], rank, -1.0).astype(bf16)
        chosen = (dot(code, spread_main) == slot_main).astype(f32).astype(bf16)
        picked = dot(chosen, main)
        hit = dot(code, spread_rest) == slot_rest
        extra = jnp.concatenate(
            [
                dot((hit & ((place % rest) // 2 == tile)).astype(f32).astype(bf16), last)
                for tile in range(tiles)
            ],
            axis=1,
        )
        total = total + columns[:, 2 + k : 3 + k] * (picked + extra)
    out_ref[...] = total.astype(bf16)


def pool_in_kernel(x_ref, gain_ref, inward_ref, pooled_ref, last_ref):
    rows, width = x_ref.shape
    block = 128
    for lower in range(0, rows, block):
        values = x_ref[lower : lower + block, :].astype(f32)
        mean = jnp.sum(values * values, axis=1, keepdims=True) / width
        normed = (values * lax.rsqrt(mean + epsilon) * gain_ref[...].astype(f32)).astype(bf16)
        pooled_ref[lower : lower + block, :] = dot(normed, inward_ref[...]).astype(bf16)
    last_ref[...] = pooled_ref[rows - HALO :, :]


def windows_kernel(
    part_ref, first_ref, pooled_ref, halo_ref, mixing_ref, scale_ref, outward_ref, *out_refs
):
    rows = pooled_ref.shape[0]
    part = part_ref[0]
    own = pooled_ref[...].astype(f32)
    total = jnp.concatenate([halo_ref[...].astype(f32), own], axis=0)
    chosen = None
    for level in range(4):
        total = total + pltpu.roll(total, 1 << level, 0)
        chosen = total if chosen is None else jnp.where(part >= level, total, chosen)
    window = jnp.left_shift(jnp.int32(2), part)
    positions = first_ref[0] + iota((rows, 1), 0)
    counts = jnp.minimum(positions + 1, window).astype(f32)
    mixed = (chosen[HALO:] / counts - own).astype(bf16)
    pooled = (dot(mixed, mixing_ref[0]) * scale_ref[...].astype(f32)).astype(bf16)
    for shift, ref in enumerate(out_refs):
        width = ref.shape[1]
        start = pl.multiple_of(((part + shift) % 4) * width, width)
        ref[...] = dot(pooled, outward_ref[:, pl.ds(start, width)]).astype(bf16)


VMEM = pl.BlockSpec(memory_space=pltpu.VMEM)
ANY = pl.BlockSpec(memory_space=pl.ANY)
SMEM = pl.BlockSpec(memory_space=pltpu.SMEM)
LARGE = pltpu.CompilerParams(vmem_limit_bytes=14 * 1024 * 1024)
SMALL = pltpu.CompilerParams(vmem_limit_bytes=12 * 1024 * 1024)


def both_halves(
    first_input,
    first_gain,
    pool_inward,
    pool_mixing,
    pool_scale,
    pool_outward,
    second_input,
    second_gain,
    route_ids,
    route_logits,
    expert_gate,
    expert_up,
    expert_down,
):
    experts = lax.axis_size("z") * lax.axis_size("y")
    width = first_input.shape[1]
    quarter = width // 4
    units = expert_gate.shape[2]
    tokens = second_input.shape[0]
    part = lax.axis_index("tp")
    part_array = part.reshape(1)
    message = jax.ShapeDtypeStruct((experts, 72, LANES), bf16)
    half_message = jax.ShapeDtypeStruct((experts // 2, 72, LANES), bf16)
    half = experts // 2

    swap = [(0, 1), (1, 0)]
    sent = pl.pallas_call(
        head_kernel,
        out_shape=message,
        in_specs=[SMEM, VMEM, VMEM, VMEM],
        out_specs=VMEM,
        compiler_params=SMALL,
        name="dispatch_rows",
    )(part_array, second_input, second_gain.reshape(1, width), route_ids.T)
    arrived = lax.all_to_all(sent, ZY, split_axis=0, concat_axis=0, tiled=True)
    gate_other = lax.ppermute(expert_gate[0], "core", swap)
    up_other = lax.ppermute(expert_up[0], "core", swap)
    down_other = lax.ppermute(expert_down[0], "core", swap)

    channels = jax.ShapeDtypeStruct((first_input.shape[0], pool_inward.shape[1]), bf16)
    pooled_in, last_rows = pl.pallas_call(
        pool_in_kernel,
        out_shape=(channels, jax.ShapeDtypeStruct((HALO, channels.shape[1]), bf16)),
        in_specs=[VMEM] * 3,
        out_specs=(VMEM,) * 2,
        compiler_params=SMALL,
        cost_estimate=pl.CostEstimate(flops=1 << 30, bytes_accessed=5 << 20, transcendentals=0),
        name="pool_in",
    )(first_input, first_gain.reshape(1, width), pool_inward)
    halo_rows = from_behind(last_rows, EP, 1)
    term = jax.ShapeDtypeStruct((first_input.shape[0], quarter), bf16)
    terms = pl.pallas_call(
        windows_kernel,
        out_shape=(term,) * 4,
        in_specs=[SMEM] * 2 + [VMEM] * 5,
        out_specs=(VMEM,) * 4,
        compiler_params=SMALL,
        cost_estimate=pl.CostEstimate(flops=1 << 29, bytes_accessed=3 << 20, transcendentals=0),
        name="windows",
    )(
        part_array,
        (lax.axis_index(EP) * first_input.shape[0]).reshape(1),
        pooled_in,
        halo_rows,
        pool_mixing,
        pool_scale.reshape(1, -1),
        pool_outward,
    )

    arrived, terms = lax.optimization_barrier((arrived, terms))
    first, second = arrived[:half], arrived[half:]
    left_a = shifted(first, "tp", 1)
    right_b = shifted(second, "tp", -1)
    left_b = shifted(second, "tp", 1)
    right_a = shifted(first, "tp", -1)
    over_a = shifted(left_a, "tp", 1)
    over_b = shifted(right_b, "tp", -1)
    term_far = shifted(terms[2], "tp", 2)

    gates = (expert_gate[0], expert_up[0], gate_other, up_other)
    products = experts * 18 * units * width
    sum_shape = jax.ShapeDtypeStruct((4, experts * 18, units), f32)

    def near(shifts, messages, earlier):
        count = len(shifts)
        return pl.pallas_call(
            functools.partial(near_kernel, shifts),
            out_shape=sum_shape,
            in_specs=[SMEM] + [VMEM] * (len(messages) + len(earlier) + 2) + [ANY] * 2,
            out_specs=VMEM,
            scratch_shapes=[
                pltpu.VMEM((experts * 18, count * quarter), bf16),
                pltpu.VMEM((count * quarter, units), bf16),
                pltpu.VMEM((count * quarter, units), bf16),
                pltpu.SemaphoreType.DMA((2 * count,)),
            ],
            compiler_params=LARGE,
            cost_estimate=pl.CostEstimate(
                flops=2 * count * products, bytes_accessed=4 << 20, transcendentals=0
            ),
        )(part_array, *messages, *earlier, *gates)

    sums = near((0,), (arrived,), ())
    sums = near((3, 1), (left_a, left_b, right_a, right_b), (sums,))
    outs = pl.pallas_call(
        far_kernel,
        out_shape=(message,) + (half_message,) * 6,
        in_specs=[SMEM] + [VMEM] * 5 + [ANY] * 2 + [VMEM, ANY],
        out_specs=(VMEM,) * 7,
        scratch_shapes=[
            pltpu.VMEM((experts * 18, quarter), bf16),
            pltpu.VMEM((experts * 18, 2 * units), bf16),
            pltpu.VMEM((quarter, units), bf16),
            pltpu.VMEM((quarter, units), bf16),
            pltpu.VMEM((units, width), bf16),
            pltpu.SemaphoreType.DMA((3,)),
        ],
        compiler_params=LARGE,
        cost_estimate=pl.CostEstimate(
            flops=6 * products, bytes_accessed=12 << 20, transcendentals=0
        ),
        name="far_quarter",
    )(part_array, over_a, over_b, sums, *gates, expert_down[0], down_other)
    own, to_right_a, to_right_b, to_left_a, to_left_b, to_over_a, to_over_b = outs

    passing_a = shifted(to_over_a, "tp", 1)
    passing_b = shifted(to_over_b, "tp", -1)
    from_left_b = shifted(to_right_b, "tp", 1)
    from_right_a = shifted(to_left_a, "tp", -1)
    from_left_a = shifted((to_right_a.astype(f32) + passing_a.astype(f32)).astype(bf16), "tp", 1)
    from_right_b = shifted((to_left_b.astype(f32) + passing_b.astype(f32)).astype(bf16), "tp", -1)
    term_left = shifted(terms[1], "tp", 1)
    term_right = shifted(terms[3], "tp", -1)
    summed = jnp.concatenate(
        [
            own[:half].astype(f32) + from_left_a.astype(f32) + from_right_a.astype(f32),
            own[half:].astype(f32) + from_left_b.astype(f32) + from_right_b.astype(f32),
        ],
        axis=0,
    ).astype(bf16)

    back = lax.all_to_all(summed, ZY, split_axis=0, concat_axis=0, tiled=True)

    back, term_far, term_left, term_right = lax.optimization_barrier(
        (back, term_far, term_left, term_right)
    )
    return pl.pallas_call(
        tail_kernel,
        out_shape=(term, jax.ShapeDtypeStruct((tokens, quarter), bf16)),
        in_specs=[VMEM] * 7,
        out_specs=(VMEM,) * 2,
        compiler_params=SMALL,
        name="combine_rows",
    )(back, route_ids.T, route_logits.T, terms[0], term_left, term_far, term_right)


def solution(mesh):
    split_mesh = Mesh(mesh.devices.reshape(8, 4, 2, 4), ("z", "y", "core", "tp"))
    placed = (
        P(EP, None),
        P(),
        P(None, "tp"),
        P("tp", None, None),
        P("tp"),
        P("tp", None),
        P(EP, None),
        P(),
        P(EP, None),
        P(EP, None),
        P(EP, None, "tp"),
        P(EP, None, "tp"),
        P(EP, "tp", None),
    )
    return jax.shard_map(
        both_halves,
        mesh=split_mesh,
        in_specs=placed,
        out_specs=(P(EP, "tp"), P(EP, "tp")),
        check_vma=False,
    )
```

```python
import functools

import jax
import jax.numpy as jnp
from jax import lax
from jax.experimental import pallas as pl
from jax.experimental.pallas import tpu as pltpu
from jax.sharding import Mesh, PartitionSpec as P

epsilon = 1e-06
EP = ("z", "y", "core")
ZY = ("z", "y")
LANES = 128
MAIN = 16
HALO = 16
f32 = jnp.float32
bf16 = jnp.bfloat16


def shifted(value, axis, steps):
    count = lax.axis_size(axis)
    return lax.ppermute(value, axis, [(i, (i + steps) % count) for i in range(count)])


def from_behind(value, axis, steps):
    count = lax.axis_size(axis)
    leading, last = (max(0, -steps), min(count, count - steps))
    return lax.ppermute(value, axis, [(source, source + steps) for source in range(leading, last)])


def iota(shape, dim):
    return lax.broadcasted_iota(jnp.int32, shape, dim)


def dot(a, b):
    return jnp.dot(a, b, preferred_element_type=f32)


def head_kernel(part_ref, x_ref, gain_ref, ids_ref, out_ref):
    tokens, width = x_ref.shape
    experts = out_ref.shape[0]
    quarter = width // 4
    total = jnp.zeros((tokens, 1), f32)
    for lower in range(0, width, quarter):
        piece = x_ref[:, lower : lower + quarter].astype(f32)
        total = total + jnp.sum(piece * piece, axis=1, keepdims=True)
    inverse = lax.rsqrt(total / width + epsilon)
    start = pl.multiple_of(part_ref[0] * quarter, quarter)
    mine = x_ref[:, pl.ds(start, quarter)].astype(f32)
    gains = gain_ref[...].astype(f32)
    tile_rows = iota(gains.shape, 0)
    first_tile = part_ref[0] * (quarter // LANES)
    gain = jnp.concatenate(
        [
            jnp.sum(jnp.where(tile_rows == first_tile + tile, gains, 0.0), axis=0, keepdims=True)
            for tile in range(quarter // LANES)
        ],
        axis=1,
    )
    normed = (mine * inverse * gain).astype(bf16)
    named = iota((experts, tokens), 0)
    member = (ids_ref[0:1, :] == named) | (ids_ref[1:2, :] == named)
    earlier = (iota((tokens, tokens), 0) < iota((tokens, tokens), 1)).astype(f32).astype(bf16)
    rank = dot(member.astype(f32).astype(bf16), earlier)
    code = jnp.where(member, rank, -1.0).astype(bf16)
    rows = experts * MAIN
    spread = (iota((rows, experts), 0) // MAIN == iota((rows, experts), 1)).astype(f32).astype(bf16)
    slot = (iota((rows, tokens), 0) % MAIN).astype(f32)
    chosen = (dot(spread, code) == slot).astype(f32).astype(bf16)
    main = dot(chosen, normed).astype(bf16)
    tiles = quarter // LANES
    for tile in range(tiles):
        out_ref[:, tile * MAIN : (tile + 1) * MAIN, :] = main[
            :, tile * LANES : (tile + 1) * LANES
        ].reshape(experts, MAIN, LANES)
    rest = 2 * tiles
    rows = experts * rest
    spread = (iota((rows, experts), 0) // rest == iota((rows, experts), 1)).astype(f32).astype(bf16)
    expanded = dot(spread, code)
    place = iota((rows, tokens), 0)
    hit = expanded == (MAIN + place % 2).astype(f32)
    summed = jnp.zeros((rows, LANES), f32)
    for tile in range(tiles):
        chosen = (hit & ((place % rest) // 2 == tile)).astype(f32).astype(bf16)
        summed = summed + dot(chosen, normed[:, tile * LANES : (tile + 1) * LANES])
    out_ref[:, tiles * MAIN :, :] = summed.reshape(experts, rest, LANES).astype(bf16)


def rest_order(sources, tiles, flip):
    size = sources * tiles * 2
    outer, inner = iota((size, size), 0), iota((size, size), 1)
    if flip:
        outer, inner = inner, outer
    tile, source, slot = outer // (2 * sources), (outer % (2 * sources)) // 2, outer % 2
    return (inner == source * 2 * tiles + tile * 2 + slot).astype(f32).astype(bf16)


def gathered_rows(x_ref, groups, sources):
    tiles = 4
    quarter = tiles * LANES
    half = sources // 2
    main_rows = sources * MAIN
    rests = []
    for index, pair in enumerate(groups):
        rest = []
        for side, (ref, first) in enumerate(pair):
            rows = half * MAIN
            for tile in range(tiles):
                block = ref[first : first + half, tile * MAIN : (tile + 1) * MAIN, :]
                lower = index * quarter + tile * LANES
                x_ref[side * rows : (side + 1) * rows, lower : lower + LANES] = block.reshape(
                    rows, LANES
                )
            rest.append(ref[first : first + half, tiles * MAIN :, :].astype(f32))
        rests.append(
            jnp.concatenate(rest, axis=0).reshape(sources * 2 * tiles, LANES).astype(bf16)
        )
    moved = dot(rest_order(sources, tiles, False), jnp.concatenate(rests, axis=1)).astype(bf16)
    for index in range(len(groups)):
        for tile in range(tiles):
            lower = index * quarter + tile * LANES
            x_ref[main_rows:, lower : lower + LANES] = moved[
                tile * 2 * sources : (tile + 1) * 2 * sources,
                index * LANES : (index + 1) * LANES,
            ]


def near_kernel(shifts, *refs):
    count = len(shifts)
    part_ref = refs[0]
    groups, place = [], 1
    for shift in shifts:
        if shift == 0:
            groups.append(((refs[place], 0), (refs[place], refs[place].shape[0] // 2)))
            place += 1
        else:
            groups.append(((refs[place], 0), (refs[place + 1], 0)))
            place += 2
    earlier_ref = None
    if shifts[0] != 0:
        earlier_ref = refs[place]
        place += 1
    g0_ref, u0_ref, g1_hbm, u1_hbm, sum_ref, x_ref, g1_ref, u1_ref, sems = refs[place:]
    quarter = 4 * LANES
    part = part_ref[0]
    starts = [pl.multiple_of(((part + shift) % 4) * quarter, quarter) for shift in shifts]
    copies = []
    for side, (source, target) in enumerate(((g1_hbm, g1_ref), (u1_hbm, u1_ref))):
        for index, start in enumerate(starts):
            copies.append(
                pltpu.make_async_copy(
                    source.at[pl.ds(start, quarter)],
                    target.at[pl.ds(index * quarter, quarter)],
                    sems.at[side * count + index],
                )
            )
    for copy in copies:
        copy.start()
    gathered_rows(x_ref, groups, x_ref.shape[0] // 18)
    for index in range(4):
        if index >= 2:
            for copy in copies[(index - 2) * count : (index - 1) * count]:
                copy.wait()
        total = None if earlier_ref is None else earlier_ref[index]
        for at, start in enumerate(starts):
            if index < 2:
                rows = (g0_ref, u0_ref)[index][pl.ds(start, quarter), :]
            else:
                rows = (g1_ref, u1_ref)[index - 2][at * quarter : (at + 1) * quarter, :]
            term = dot(x_ref[:, at * quarter : (at + 1) * quarter], rows)
            total = term if total is None else total + term
        sum_ref[index] = total


def far_kernel(
    part_ref, oa_ref, ob_ref, sum_ref, g0_ref, u0_ref, g1_hbm, u1_hbm, d0_ref, d1_hbm,
    oa_out, ob_out, hidden_ref,
    x_ref, g1_ref, u1_ref, d1_ref, sems,
):
    half = oa_ref.shape[0]
    sources = 2 * half
    tiles = 4
    quarter = tiles * LANES
    units = g0_ref.shape[1]
    part = part_ref[0]
    starts = [pl.multiple_of(((part + shift) % 4) * quarter, quarter) for shift in (2, 3, 1, 0)]
    far = pl.ds(starts[0], quarter)
    copies = [
        pltpu.make_async_copy(g1_hbm.at[far], g1_ref, sems.at[0]),
        pltpu.make_async_copy(u1_hbm.at[far], u1_ref, sems.at[1]),
        pltpu.make_async_copy(d1_hbm, d1_ref, sems.at[2]),
    ]
    for copy in copies:
        copy.start()
    gathered_rows(x_ref, (((oa_ref, 0), (ob_ref, 0)),), sources)
    x = x_ref[...]
    for side in range(2):
        if side == 0:
            gate_rows, up_rows = g0_ref[far, :], u0_ref[far, :]
        else:
            copies[0].wait()
            copies[1].wait()
            gate_rows, up_rows = g1_ref[...], u1_ref[...]
        gate = sum_ref[2 * side] + dot(x, gate_rows)
        up = sum_ref[2 * side + 1] + dot(x, up_rows)
        hidden_ref[:, side * units : (side + 1) * units] = (
            gate / (1.0 + jnp.exp(-gate)) * up
        ).astype(bf16)
    copies[2].wait()
    down_terms(part, (2,), hidden_ref, d0_ref, d1_ref, (((oa_out, 0), (ob_out, 0)),), sources)


def down_terms(part, shifts, hidden_ref, d0_ref, d1_ref, targets, sources):
    tiles = 4
    quarter = tiles * LANES
    half = sources // 2
    units = d0_ref.shape[0]
    main_rows = sources * MAIN
    rests = []
    for shift, pair in zip(shifts, targets):
        start = pl.multiple_of(((part + shift) % 4) * quarter, quarter)
        result = (
            dot(hidden_ref[:, :units], d0_ref[:, pl.ds(start, quarter)])
            + dot(hidden_ref[:, units:], d1_ref[:, pl.ds(start, quarter)])
        ).astype(bf16)
        rows = half * MAIN
        for side, (ref, first) in enumerate(pair):
            for tile in range(tiles):
                ref[first : first + half, tile * MAIN : (tile + 1) * MAIN, :] = result[
                    side * rows : (side + 1) * rows, tile * LANES : (tile + 1) * LANES
                ].reshape(half, MAIN, LANES)
        rests.append(
            jnp.concatenate(
                [result[main_rows:, tile * LANES : (tile + 1) * LANES] for tile in range(tiles)],
                axis=0,
            )
        )
    moved = dot(rest_order(sources, tiles, True), jnp.concatenate(rests, axis=1))
    for index, pair in enumerate(targets):
        block = moved[:, index * LANES : (index + 1) * LANES].reshape(sources, 2 * tiles, LANES)
        for side, (ref, first) in enumerate(pair):
            ref[first : first + half, tiles * MAIN :, :] = block[
                side * half : (side + 1) * half
            ].astype(bf16)


def rest_kernel(
    part_ref, hidden_ref, d0_ref, d1_ref, own_out, ra_out, rb_out, la_out, lb_out
):
    half = ra_out.shape[0]
    targets = (
        ((la_out, 0), (lb_out, 0)),
        ((ra_out, 0), (rb_out, 0)),
        ((own_out, 0), (own_out, half)),
    )
    down_terms(part_ref[0], (3, 1, 0), hidden_ref, d0_ref, d1_ref, targets, 2 * half)


def prepare_kernel(ids_ref, logits_ref, main_ref, rest_ref, shares_ref):
    tokens = ids_ref.shape[1]
    rows = main_ref.shape[2]
    experts = rows // MAIN
    rest = rest_ref.shape[2] // experts
    logits = logits_ref[...]
    shares = jax.nn.sigmoid(logits - jnp.concatenate([logits[1:2], logits[0:1]], axis=0))
    columns = jnp.transpose(
        jnp.concatenate(
            [shares, ids_ref[...].astype(f32), jnp.zeros((4, tokens), f32)], axis=0
        )
    )
    shares_ref[...] = columns
    named = iota((tokens, experts), 1).astype(f32)
    members = [columns[:, 2 + k : 3 + k] == named for k in range(2)]
    earlier = (iota((tokens, tokens), 1) < iota((tokens, tokens), 0)).astype(f32).astype(bf16)
    rank = dot(earlier, (members[0] | members[1]).astype(f32).astype(bf16))
    spread_main = (
        (iota((experts, rows), 1) // MAIN == iota((experts, rows), 0)).astype(f32).astype(bf16)
    )
    slot_main = (iota((tokens, rows), 1) % MAIN).astype(f32)
    rest_rows = experts * rest
    spread_rest = (
        (iota((experts, rest_rows), 1) // rest == iota((experts, rest_rows), 0))
        .astype(f32)
        .astype(bf16)
    )
    place = iota((tokens, rest_rows), 1)
    slot_rest = (MAIN + place % 2).astype(f32)
    for k in range(2):
        code = jnp.where(members[k], rank, -1.0).astype(bf16)
        main_ref[k] = (dot(code, spread_main) == slot_main).astype(f32).astype(bf16)
        rest_ref[k] = (dot(code, spread_rest) == slot_rest).astype(f32).astype(bf16)


def tail_kernel(back_ref, main_ref, rest_ref, shares_ref, out_ref):
    experts = back_ref.shape[0]
    tiles = out_ref.shape[1] // LANES
    rows = experts * MAIN
    main = jnp.concatenate(
        [
            back_ref[:, tile * MAIN : (tile + 1) * MAIN, :].reshape(rows, LANES)
            for tile in range(tiles)
        ],
        axis=1,
    )
    last = back_ref[:, tiles * MAIN :, :].astype(f32).reshape(-1, LANES)
    owner = (iota(last.shape, 0) % (2 * tiles)) // 2
    last = jnp.concatenate(
        [jnp.where(owner == tile, last, 0.0) for tile in range(tiles)], axis=1
    ).astype(bf16)
    total = None
    for k in range(2):
        extra = dot(rest_ref[k], last)
        term = shares_ref[:, k : k + 1] * (dot(main_ref[k], main) + extra)
        total = term if total is None else total + term
    out_ref[...] = total.astype(bf16)


def pool_in_kernel(x_ref, gain_ref, inward_ref, pooled_ref, last_ref):
    rows, width = x_ref.shape
    block = 128
    gains = gain_ref[...].astype(f32)
    gain = jnp.concatenate([gains[tile : tile + 1] for tile in range(width // LANES)], axis=1)
    for lower in range(0, rows, block):
        values = x_ref[lower : lower + block, :].astype(f32)
        mean = jnp.sum(values * values, axis=1, keepdims=True) / width
        normed = (values * lax.rsqrt(mean + epsilon) * gain).astype(bf16)
        pooled_ref[lower : lower + block, :] = dot(normed, inward_ref[...]).astype(bf16)
    last_ref[...] = pooled_ref[rows - HALO :, :]


def windows_kernel(part_ref, first_ref, pooled_ref, halo_ref, mixing_ref, scale_ref, out_ref):
    rows = pooled_ref.shape[0]
    part = part_ref[0]
    own = pooled_ref[...].astype(f32)
    total = jnp.concatenate([halo_ref[...].astype(f32), own], axis=0)
    chosen = None
    for level in range(4):
        total = total + pltpu.roll(total, 1 << level, 0)
        chosen = total if chosen is None else jnp.where(part >= level, total, chosen)
    window = jnp.left_shift(jnp.int32(2), part)
    positions = first_ref[0] + iota((rows, 1), 0)
    counts = jnp.minimum(positions + 1, window).astype(f32)
    mixed = (chosen[HALO:] / counts - own).astype(bf16)
    out_ref[...] = (dot(mixed, mixing_ref[0]) * scale_ref[...].astype(f32)).astype(bf16)


def pool_out_kernel(*refs):
    total = dot(refs[0][...], refs[4][...])
    for channels, weights in zip(refs[1:4], refs[5:8]):
        total = total + dot(channels[...], weights[...])
    refs[8][...] = total.astype(bf16)


def sum_kernel(own_ref, la_ref, ra_ref, lb_ref, rb_ref, out_ref):
    half = la_ref.shape[0]
    for first, refs in ((0, (la_ref, ra_ref)), (half, (lb_ref, rb_ref))):
        total = own_ref[first : first + half].astype(f32)
        out_ref[first : first + half] = (
            total + refs[0][...].astype(f32) + refs[1][...].astype(f32)
        ).astype(bf16)


VMEM = pl.BlockSpec(memory_space=pltpu.VMEM)
ANY = pl.BlockSpec(memory_space=pl.ANY)
SMEM = pl.BlockSpec(memory_space=pltpu.SMEM)
LARGE = pltpu.CompilerParams(vmem_limit_bytes=14 * 1024 * 1024)
SMALL = pltpu.CompilerParams(vmem_limit_bytes=12 * 1024 * 1024)


def both_halves(
    first_input,
    first_gain,
    pool_inward,
    pool_mixing,
    pool_scale,
    pool_outward,
    second_input,
    second_gain,
    route_ids,
    route_logits,
    expert_gate,
    expert_up,
    expert_down,
):
    experts = lax.axis_size("z") * lax.axis_size("y")
    width = first_input.shape[1]
    quarter = width // 4
    units = expert_gate.shape[2]
    tokens = second_input.shape[0]
    part = lax.axis_index("tp")
    part_array = part.reshape(1)
    message = jax.ShapeDtypeStruct((experts, 72, LANES), bf16)
    half_message = jax.ShapeDtypeStruct((experts // 2, 72, LANES), bf16)
    half = experts // 2

    swap = [(0, 1), (1, 0)]
    sent = pl.pallas_call(
        head_kernel,
        out_shape=message,
        in_specs=[SMEM, VMEM, VMEM, VMEM],
        out_specs=VMEM,
        compiler_params=SMALL,
        name="dispatch_rows",
    )(part_array, second_input, second_gain.reshape(width // LANES, LANES), route_ids.T)
    sent, pool_outward = lax.optimization_barrier((sent, pool_outward))
    arrived = lax.all_to_all(sent, ZY, split_axis=0, concat_axis=0, tiled=True)
    gate_other = lax.ppermute(expert_gate[0], "core", swap)
    up_other = lax.ppermute(expert_up[0], "core", swap)
    down_other = lax.ppermute(expert_down[0], "core", swap)

    channels = jax.ShapeDtypeStruct((first_input.shape[0], pool_inward.shape[1]), bf16)
    pooled_in, last_rows = pl.pallas_call(
        pool_in_kernel,
        out_shape=(channels, jax.ShapeDtypeStruct((HALO, channels.shape[1]), bf16)),
        in_specs=[VMEM] * 3,
        out_specs=(VMEM,) * 2,
        compiler_params=SMALL,
        cost_estimate=pl.CostEstimate(flops=1 << 30, bytes_accessed=5 << 20, transcendentals=0),
        name="pool_in",
    )(first_input, first_gain.reshape(width // LANES, LANES), pool_inward)
    halo_rows = from_behind(last_rows, EP, 1)
    slices = [
        lax.dynamic_slice_in_dim(pool_outward, ((part + shift) % 4) * quarter, quarter, 1)
        for shift in range(4)
    ]
    outward = [shifted(slices[shift], "tp", shift) for shift in (1, 2, 3)]

    arrived, pooled_in = lax.optimization_barrier((arrived, pooled_in))
    first, second = arrived[:half], arrived[half:]
    left_a = shifted(first, "tp", 1)
    right_b = shifted(second, "tp", -1)
    left_b = shifted(second, "tp", 1)
    right_a = shifted(first, "tp", -1)
    over_a = shifted(left_a, "tp", 1)
    over_b = shifted(right_b, "tp", -1)

    gates = (expert_gate[0], expert_up[0], gate_other, up_other)
    products = experts * 18 * units * width
    sum_shape = jax.ShapeDtypeStruct((4, experts * 18, units), f32)

    def near(shifts, messages, earlier):
        count = len(shifts)
        return pl.pallas_call(
            functools.partial(near_kernel, shifts),
            out_shape=sum_shape,
            in_specs=[SMEM] + [VMEM] * (len(messages) + len(earlier) + 2) + [ANY] * 2,
            out_specs=VMEM,
            scratch_shapes=[
                pltpu.VMEM((experts * 18, count * quarter), bf16),
                pltpu.VMEM((count * quarter, units), bf16),
                pltpu.VMEM((count * quarter, units), bf16),
                pltpu.SemaphoreType.DMA((2 * count,)),
            ],
            compiler_params=LARGE,
            cost_estimate=pl.CostEstimate(
                flops=2 * count * products, bytes_accessed=4 << 20, transcendentals=0
            ),
        )(part_array, *messages, *earlier, *gates)

    sums = near((0,), (arrived,), ())
    sums = near((3, 1), (left_a, left_b, right_a, right_b), (sums,))
    to_over_a, to_over_b, hidden = pl.pallas_call(
        far_kernel,
        out_shape=(half_message,) * 2
        + (jax.ShapeDtypeStruct((experts * 18, 2 * units), bf16),),
        in_specs=[SMEM] + [VMEM] * 5 + [ANY] * 2 + [VMEM, ANY],
        out_specs=(VMEM,) * 3,
        scratch_shapes=[
            pltpu.VMEM((experts * 18, quarter), bf16),
            pltpu.VMEM((quarter, units), bf16),
            pltpu.VMEM((quarter, units), bf16),
            pltpu.VMEM((units, width), bf16),
            pltpu.SemaphoreType.DMA((3,)),
        ],
        compiler_params=LARGE,
        cost_estimate=pl.CostEstimate(
            flops=3 * products, bytes_accessed=12 << 20, transcendentals=0
        ),
        name="far_quarter",
    )(part_array, over_a, over_b, sums, *gates, expert_down[0], down_other)
    own, to_right_a, to_right_b, to_left_a, to_left_b = pl.pallas_call(
        rest_kernel,
        out_shape=(message,) + (half_message,) * 4,
        in_specs=[SMEM] + [VMEM] * 3,
        out_specs=(VMEM,) * 5,
        compiler_params=LARGE,
        cost_estimate=pl.CostEstimate(
            flops=3 * products, bytes_accessed=8 << 20, transcendentals=0
        ),
        name="rest_terms",
    )(part_array, hidden, expert_down[0], down_other)

    passing_a = shifted(to_over_a, "tp", 1)
    passing_b = shifted(to_over_b, "tp", -1)
    from_left_b = shifted(to_right_b, "tp", 1)
    from_right_a = shifted(to_left_a, "tp", -1)
    pooled_in, halo_rows, passing_a, passing_b = lax.optimization_barrier(
        (pooled_in, halo_rows, passing_a, passing_b)
    )
    from_left_a = shifted((to_right_a.astype(f32) + passing_a.astype(f32)).astype(bf16), "tp", 1)
    from_right_b = shifted((to_left_b.astype(f32) + passing_b.astype(f32)).astype(bf16), "tp", -1)
    pooled = pl.pallas_call(
        windows_kernel,
        out_shape=channels,
        in_specs=[SMEM] * 2 + [VMEM] * 4,
        out_specs=VMEM,
        compiler_params=SMALL,
        cost_estimate=pl.CostEstimate(flops=1 << 28, bytes_accessed=1 << 20, transcendentals=0),
        name="windows",
    )(
        part_array,
        (lax.axis_index(EP) * first_input.shape[0]).reshape(1),
        pooled_in,
        halo_rows,
        pool_mixing,
        pool_scale.reshape(1, -1),
    )
    summed = pl.pallas_call(
        sum_kernel,
        out_shape=message,
        in_specs=[VMEM] * 5,
        out_specs=VMEM,
        compiler_params=SMALL,
        name="ring_sum",
    )(own, from_left_a, from_right_a, from_left_b, from_right_b)
    summed, pooled = lax.optimization_barrier((summed, pooled))
    back = lax.all_to_all(summed, ZY, split_axis=0, concat_axis=0, tiled=True)
    pooled_far = shifted(pooled, "tp", 2)
    pooled_sides = [shifted(pooled, "tp", shift) for shift in (1, 3)]
    others = [pooled_sides[0], pooled_far, pooled_sides[1]]
    first_out = pl.pallas_call(
        pool_out_kernel,
        out_shape=jax.ShapeDtypeStruct((first_input.shape[0], quarter), bf16),
        in_specs=[VMEM] * 8,
        out_specs=VMEM,
        compiler_params=SMALL,
        cost_estimate=pl.CostEstimate(flops=1 << 29, bytes_accessed=2 << 20, transcendentals=0),
        name="pool_out",
    )(pooled, *others, slices[0], *outward)
    chosen_main, chosen_rest, shares = pl.pallas_call(
        prepare_kernel,
        out_shape=(
            jax.ShapeDtypeStruct((2, tokens, experts * MAIN), bf16),
            jax.ShapeDtypeStruct((2, tokens, experts * 8), bf16),
            jax.ShapeDtypeStruct((tokens, 8), f32),
        ),
        in_specs=[VMEM] * 2,
        out_specs=(VMEM,) * 3,
        compiler_params=SMALL,
        name="combine_prepare",
    )(route_ids.T, route_logits.T)
    second_out = pl.pallas_call(
        tail_kernel,
        out_shape=jax.ShapeDtypeStruct((tokens, quarter), bf16),
        in_specs=[VMEM] * 4,
        out_specs=VMEM,
        compiler_params=SMALL,
        name="combine_rows",
    )(back, chosen_main, chosen_rest, shares)
    return (first_out, second_out)


def solution(mesh):
    split_mesh = Mesh(mesh.devices.reshape(8, 4, 2, 4), ("z", "y", "core", "tp"))
    placed = (
        P(EP, None),
        P(),
        P(None, "tp"),
        P("tp", None, None),
        P("tp"),
        P("tp", None),
        P(EP, None),
        P(),
        P(EP, None),
        P(EP, None),
        P(EP, None, "tp"),
        P(EP, None, "tp"),
        P(EP, "tp", None),
    )
    return jax.shard_map(
        both_halves,
        mesh=split_mesh,
        in_specs=placed,
        out_specs=(P(EP, "tp"), P(EP, "tp")),
        check_vma=False,
    )
```
